32 devices in a mesh: ep: 8 (over z, core), tp: 4 (over y, x).
Axes of the slice: x: 2, y: 2, z: 4, core: 2. Of those that a mesh axis runs over, the one named last changes fastest.
Arguments:
- tokens: bfloat16 [2048, 2048], P('ep'), may hold values from -6 to 6
- gate_proj: bfloat16 [8, 2048, 4096], P('ep', None, 'tp'), may hold values from -0.125 to 0.125
- up_proj: bfloat16 [8, 2048, 4096], P('ep', None, 'tp'), may hold values from -0.125 to 0.125
- down_proj: bfloat16 [8, 4096, 2048], P('ep', 'tp'), may hold values from -0.09375 to 0.09375
- side_input_weight: bfloat16 [2048, 1024], P(None, 'tp'), may hold values from -0.125 to 0.125
- dense_out: bfloat16 [1024, 2048], P(None, 'tp'), may hold values from -0.1875 to 0.1875
- dense_gate: bfloat16 [2048], replicated, may hold values from -0.125 to 0.125
- chosen_rows: int32 [8, 256], P(None, 'ep'), may hold values from 0 to 255, as said below
- choice_weights: float32 [8, 256], P(None, 'ep'), may hold values from 0.25 to 1
Outputs:
- mixed: bfloat16 [2048, 2048], P('ep', 'tp')
The draws below stay inside these ranges and needn't reach their ends.
Inputs may be any that keep to these rules, and one draw needn't show every extreme that they name: `chosen_rows`: for each expert and each block of 32 columns (one index of ep), the 32 rows are distinct rows of that index's 256 tokens; every expert reads exactly 32 tokens of every index.
All inputs are finite; a program needn't handle non-finite values.
Results may differ from the reference program's by a relative error of at most 0.015.
Values may be sent and summed in bfloat16 or wider, within the bound.
No kernel may reach another device: no remote copies, remote signals or barrier semaphores. Data moves between devices by JAX's collectives and lax.ppermute only.
A program may use at most 64 MiB of HBM per device.

```python
import jax
import jax.numpy as jnp
from jax import lax

D = 2048
FF = 4096
DENSE_FF = 1024
TOK_DEV = 256
SLOT = 32
EXPERTS = 8
CAP = 256
TOKENS = 2048
N_TP = 4


def draw_chosen_rows(key, part):
    block_list = TOKENS // TOK_DEV
    keys = jax.random.split(jax.random.fold_in(key, 17), EXPERTS * block_list)
    orders = jax.vmap(lambda k: jax.random.permutation(k, TOK_DEV))(keys)
    picked = orders[:, :SLOT].astype(jnp.int32)
    return picked.reshape(EXPERTS, block_list * SLOT)


def level_of(stream_key, extent, shards, least, largest):
    def one(axis_at, parts):
        draws = jax.random.uniform(jax.random.fold_in(jax.random.fold_in(stream_key, 6), axis_at), (parts,), jnp.float32, least / len(shards), largest / len(shards))
        return jnp.repeat(jnp.exp(draws), extent[axis_at] // parts).reshape((-1,) + (1,) * (len(extent) - axis_at - 1))

    level = one(*shards[0])
    for cut in shards[1:]:
        level = level * one(*cut)
    return level


def gaussian(rng, dims, width, bound, cuts=(), dtype=jnp.bfloat16):
    factor_of = level_of(rng, dims, cuts, -0.22, 0.18) if cuts else 1.0
    values = jax.random.normal(rng, dims, jnp.float32) * width * factor_of
    return jnp.minimum(jnp.maximum(values, -bound), bound).astype(dtype)


def setup_inputs(seed: int = 0) -> dict:
    splits = jax.random.split(jax.random.key(seed), 10)
    return {
        "tokens": gaussian(splits[0], (TOKENS, D), 1.0, 6.0, ((0, 8),)),
        "gate_proj": gaussian(splits[1], (EXPERTS, D, FF), D ** -0.5, 0.125, ((0, 8), (2, 4))),
        "up_proj": gaussian(splits[2], (EXPERTS, D, FF), D ** -0.5, 0.125, ((0, 8), (2, 4))),
        "down_proj": gaussian(splits[3], (EXPERTS, FF, D), FF ** -0.5, 0.09375, ((0, 8), (1, 4))),
        "side_input_weight": gaussian(splits[4], (D, DENSE_FF), D ** -0.5, 0.125, ((1, 4),)),
        "dense_out": gaussian(splits[5], (DENSE_FF, D), DENSE_FF ** -0.5, 0.1875, ((1, 4),)),
        "dense_gate": gaussian(splits[6], (D,), D ** -0.5, 0.125),
        "chosen_rows": draw_chosen_rows(jax.random.fold_in(splits[9], 71), 0),
        "choice_weights": jnp.clip(0.25 + 0.75 * jax.random.uniform(splits[8], (EXPERTS, CAP), jnp.float32) ** level_of(splits[8], (EXPERTS, CAP), ((1, 8),), -0.2, 0.2), 0.25, 1.0),
    }


def reference(tokens, gate_proj, up_proj, down_proj, side_input_weight, dense_out, dense_gate, chosen_rows, choice_weights):
    token_id = ((jnp.arange(CAP) // SLOT) * TOK_DEV).astype(jnp.int32)[None, :] + chosen_rows.astype(jnp.int32)

    def one_expert(routed, inputs):
        w_gate, w_up, w_down, ids, weights = inputs
        picked = jnp.take(tokens, ids, axis=0)
        gate_val = jnp.dot(picked, w_gate, preferred_element_type=jnp.float32)
        up_val = jnp.dot(picked, w_up, preferred_element_type=jnp.float32)
        hidden = (jax.nn.silu(gate_val) * up_val).astype(jnp.bfloat16)
        block_list = hidden.reshape(CAP, N_TP, FF // N_TP).astype(jnp.float32)
        down_weight_blocks = w_down.reshape(N_TP, FF // N_TP, D).astype(jnp.float32)
        part = jnp.einsum('lyk,yka->yla', block_list, down_weight_blocks, precision=lax.Precision.HIGHEST)
        part = lax.optimization_barrier(part.astype(jnp.bfloat16)).astype(jnp.float32)
        expert_out = jnp.sum(part, axis=0).astype(jnp.bfloat16)
        routed = routed.at[ids].add(weights[:, None] * expert_out.astype(jnp.float32))
        return routed, None

    routed, _ = lax.scan(one_expert, jnp.zeros((TOKENS, D), jnp.float32),
                         (gate_proj, up_proj, down_proj, token_id, choice_weights))
    dense_hidden = jax.nn.silu(jnp.dot(tokens, side_input_weight, preferred_element_type=jnp.float32)).astype(jnp.bfloat16)
    dense_val = jnp.dot(dense_hidden, dense_out, preferred_element_type=jnp.float32)
    side_gate = jax.nn.sigmoid(jnp.dot(tokens, dense_gate, preferred_element_type=jnp.float32))
    return (routed + side_gate[:, None] * dense_val).astype(jnp.bfloat16)
```

```python
import functools

import jax
import jax.numpy as jnp
from jax import lax
from jax.experimental import pallas as pl
from jax.experimental.pallas import tpu as pltpu
from jax.sharding import PartitionSpec as P

BF = jnp.bfloat16
F32 = jnp.float32


def call(body, outs, limit_mib, name):
    return pl.pallas_call(
        body,
        out_shape=outs,
        compiler_params=pltpu.CompilerParams(vmem_limit_bytes=limit_mib << 20),
        name=name,
    )


def shape(dims, dtype):
    return jax.ShapeDtypeStruct(dims, dtype)


def dot(a, b):
    return jnp.dot(a, b, preferred_element_type=F32)


def slot_rows(table_ref, experts):
    me = lax.axis_index("ep")
    order = list(range(0, experts, 2)) + list(range(1, experts, 2))
    return jnp.concatenate([table_ref[pl.ds(me ^ r, 1), :] for r in order], axis=1)


def pick_body(experts, chosen, weights, tokens, keep, give, comb):
    rows = tokens.shape[0]
    width = keep.shape[1]
    half = keep.shape[0]
    at = pl.multiple_of(lax.axis_index("tp") * width, width)
    slots = slot_rows(chosen, experts)
    hit = lax.broadcasted_iota(jnp.int32, (rows, slots.shape[1]), 0) == slots
    sel = jnp.where(hit, 1.0, 0.0).astype(BF)
    got = lax.dot_general(
        sel, tokens[:, pl.ds(at, width)], (((0,), (0,)), ((), ())), preferred_element_type=F32
    ).astype(BF)
    keep[...] = got[:half]
    give[...] = got[half:]
    w = slot_rows(weights, experts)
    high = w.astype(BF).astype(F32)
    n = slots.shape[1]
    comb[:, :n] = jnp.where(hit, high, 0.0).astype(BF)
    comb[:, n:] = jnp.where(hit, w - high, 0.0).astype(BF)


def silu(v):
    return v / (1.0 + jnp.exp(-v))


def dense_in_body(tokens, w_in, w_gate, hidden, gate):
    t = tokens[...]
    hidden[...] = silu(dot(t, w_in[...])).astype(BF)
    g = jnp.sum(t.astype(F32) * w_gate[...].astype(F32), axis=1, keepdims=True)
    gate[...] = jax.nn.sigmoid(g)


def first_body(own, c1, c2, w_gate, w_up, acc_gate, acc_up):
    tp = lax.axis_index("tp")
    width = own.shape[1]
    gate = up = 0.0
    for j, chunk in enumerate((own, c1, c2)):
        at = pl.ds(pl.multiple_of((tp ^ j) * width, width), width)
        v = chunk[...]
        gate = gate + dot(v, w_gate[at, :])
        up = up + dot(v, w_up[at, :])
    acc_gate[...] = gate
    acc_up[...] = up


def last_body(c3, acc_gate, acc_up, w_gate, w_up, w_down, p0, p1, p2, p3):
    tp = lax.axis_index("tp")
    width = c3.shape[1]
    at = pl.ds(pl.multiple_of((tp ^ 3) * width, width), width)
    v = c3[...]
    gate = acc_gate[...] + dot(v, w_gate[at, :])
    up = acc_up[...] + dot(v, w_up[at, :])
    hidden = (silu(gate) * up).astype(BF)
    for j, out in ((3, p3), (1, p1), (2, p2), (0, p0)):
        cols = pl.ds(pl.multiple_of((tp ^ j) * width, width), width)
        out[...] = dot(hidden, w_down[:, cols]).astype(BF)


def dense_out_body(h0, h1, h2, h3, w_out, gate, val):
    tp = lax.axis_index("tp")
    width = h0.shape[1]
    total = 0.0
    for j, h in enumerate((h0, h1, h2, h3)):
        rows = pl.ds(pl.multiple_of((tp ^ j) * width, width), width)
        total = total + dot(h[...], w_out[rows, :])
    val[...] = gate[...] * total


def combine_body(own, other, comb, val, out):
    half = own.shape[0]
    n = 2 * half
    a, b = own[...], other[...]
    total = val[...]
    for base in (0, n):
        total = total + dot(comb[:, base : base + half], a)
        total = total + dot(comb[:, base + half : base + n], b)
    out[...] = total.astype(BF)


def swap(v, axis, size, k):
    return lax.ppermute(v, axis, [(i, i ^ k) for i in range(size)])


def fast(
    tokens,
    gate_proj,
    up_proj,
    down_proj,
    side_input_weight,
    dense_out,
    dense_gate,
    chosen_rows,
    choice_weights,
):
    experts, slots = chosen_rows.shape
    tp_size = lax.axis_size("tp")
    rows, model = tokens.shape
    width = model // tp_size
    zs = experts // 2
    half = zs * slots
    w_gate, w_up, w_down = gate_proj[0], up_proj[0], down_proj[0]
    ff = w_gate.shape[1]

    keep, give, comb = call(
        functools.partial(pick_body, experts),
        (shape((half, width), BF), shape((half, width), BF), shape((rows, 4 * half), BF)),
        8,
        "pick",
    )(chosen_rows, choice_weights, tokens)
    got = swap(give, "ep", experts, 1)
    blocks = jnp.stack([keep.reshape(zs, slots, width), got.reshape(zs, slots, width)], axis=1)
    arrived = [blocks[0]] + [swap(blocks[k], "ep", experts, 2 * k) for k in range(1, zs)]
    arrived = jnp.concatenate(arrived, axis=0).reshape(2 * half, width)

    hidden_own, side_gate = call(
        dense_in_body,
        (shape((rows, side_input_weight.shape[1]), BF), shape((rows, 1), F32)),
        8,
        "dense_in",
    )(tokens, side_input_weight, dense_gate.reshape(1, model))

    chunks = [arrived] + [swap(arrived, "tp", tp_size, j) for j in (1, 2, 3)]
    accs = call(
        first_body,
        (shape((2 * half, ff), F32), shape((2 * half, ff), F32)),
        16,
        "first",
    )(*chunks[:3], w_gate, w_up)
    part = call(last_body, (shape((2 * half, width), BF),) * 4, 16, "last")(
        chunks[3], *accs, w_gate, w_up, w_down
    )
    sent = {j: swap(part[j], "tp", tp_size, j) for j in (3, 1, 2)}
    summed = (
        part[0].astype(F32) + sent[1].astype(F32) + sent[2].astype(F32) + sent[3].astype(F32)
    ).astype(BF)
    blocks = summed.reshape(zs, 2, slots, width)
    back = [blocks[0]] + [swap(blocks[k], "ep", experts, 2 * k) for k in range(1, zs)]
    mine = jnp.concatenate([b[0] for b in back], axis=0)
    theirs = swap(jnp.concatenate([b[1] for b in back], axis=0), "ep", experts, 1)

    hiddens = [hidden_own] + [swap(hidden_own, "tp", tp_size, j) for j in (1, 2, 3)]
    val = call(dense_out_body, shape((rows, width), F32), 8, "dense_out")(
        *hiddens, dense_out, side_gate
    )
    return call(combine_body, shape((rows, width), BF), 8, "combine")(mine, theirs, comb, val)


def general(
    tokens,
    gate_proj,
    up_proj,
    down_proj,
    side_input_weight,
    dense_out,
    dense_gate,
    chosen_rows,
    choice_weights,
):
    tok_rows = tokens.shape[0]
    width = tokens.shape[1] // lax.axis_size("tp")
    column_position = lax.axis_index("tp") * width
    own_cols = lax.dynamic_slice_in_dim(tokens, column_position, width, 1)
    expert_count, slot_rows = chosen_rows.shape
    capacity = expert_count * slot_rows
    picked = jnp.take(own_cols, chosen_rows.reshape(-1), axis=0).reshape(
        expert_count, slot_rows, width
    )
    arrived = lax.all_to_all(picked, "ep", split_axis=0, concat_axis=1, tiled=True).reshape(
        capacity, width
    )
    w_gate = gate_proj[0]
    w_up = up_proj[0]
    w_down = down_proj[0]
    piece = lax.all_gather(arrived, "tp", axis=1, tiled=True)
    gate_val = jnp.dot(piece, w_gate, preferred_element_type=jnp.float32)
    up_val = jnp.dot(piece, w_up, preferred_element_type=jnp.float32)
    hidden = (jax.nn.silu(gate_val) * up_val).astype(jnp.bfloat16)
    summed = lax.psum_scatter(
        lax.dot_general(
            w_down, hidden, (((0,), (1,)), ((), ())), preferred_element_type=jnp.float32
        ).astype(jnp.bfloat16),
        "tp",
        scatter_dimension=0,
        tiled=True,
    )
    returned = lax.all_to_all(summed, "ep", split_axis=1, concat_axis=1, tiled=True)
    hits = (
        chosen_rows.reshape(-1)[:, None] == jnp.arange(tok_rows, dtype=jnp.int32)[None, :]
    ).astype(jnp.bfloat16)
    scaled = returned.astype(jnp.float32) * choice_weights.reshape(-1)[None, :]
    high_part = scaled.astype(jnp.bfloat16)
    lower_half = (scaled - high_part.astype(jnp.float32)).astype(jnp.bfloat16)
    contract = (((0,), (1,)), ((), ()))
    routed = lax.dot_general(
        hits, high_part, contract, preferred_element_type=jnp.float32
    ) + lax.dot_general(hits, lower_half, contract, preferred_element_type=jnp.float32)
    dense_hidden = jax.nn.silu(
        jnp.dot(tokens, side_input_weight, preferred_element_type=jnp.float32)
    ).astype(jnp.bfloat16)
    dense_val = jnp.dot(
        lax.all_gather(dense_hidden, "tp", axis=1, tiled=True),
        dense_out,
        preferred_element_type=jnp.float32,
    )
    side_gate = jax.nn.sigmoid(jnp.dot(tokens, dense_gate, preferred_element_type=jnp.float32))
    return (routed + side_gate[:, None] * dense_val).astype(jnp.bfloat16)


def per_device(tokens, gate_proj, *rest):
    experts = lax.axis_size("ep")
    fits = (
        lax.axis_size("tp") == 4
        and experts >= 4
        and experts & (experts - 1) == 0
        and tokens.shape[1] % (4 * 128) == 0
        and gate_proj.shape[2] % 128 == 0
        and rest[2].shape[1] % 128 == 0
        and tokens.shape[0] <= 512
        and rest[5].size <= 512
    )
    return (fast if fits else general)(tokens, gate_proj, *rest)


def solution(mesh):
    placed = (
        P("ep", None),
        P("ep", None, "tp"),
        P("ep", None, "tp"),
        P("ep", "tp", None),
        P(None, "tp"),
        P(None, "tp"),
        P(),
        P(None, "ep"),
        P(None, "ep"),
    )
    return jax.shard_map(
        per_device, mesh=mesh, in_specs=placed, out_specs=P("ep", "tp"), check_vma=False
    )
```

```python
import functools

import jax
import jax.numpy as jnp
from jax import lax
from jax.experimental import pallas as pl
from jax.experimental.pallas import tpu as pltpu
from jax.sharding import PartitionSpec as P

BF = jnp.bfloat16
F32 = jnp.float32


def call(body, outs, limit_mib):
    return pl.pallas_call(
        body, out_shape=outs, compiler_params=pltpu.CompilerParams(vmem_limit_bytes=limit_mib << 20)
    )


def shape(dims, dtype):
    return jax.ShapeDtypeStruct(dims, dtype)


def dot(a, b):
    return jnp.dot(a, b, preferred_element_type=F32)


def hbm():
    return pl.BlockSpec(memory_space=pltpu.HBM)


def in_hbm(*arrays):
    return [pltpu.with_memory_space_constraint(a, pltpu.HBM) for a in arrays]


def vmem():
    return pl.BlockSpec(memory_space=pltpu.VMEM)


def table_row(table, ranks):
    me = lax.axis_index("ep")
    return jnp.concatenate([table[pl.ds(me ^ r, 1), :] for r in ranks], axis=1)


def hits(table, ranks, rows):
    slots = table_row(table, ranks)
    return lax.broadcasted_iota(jnp.int32, (rows, slots.shape[1]), 0) == slots


def select(hit, values):
    sel = jnp.where(hit, 1.0, 0.0).astype(BF)
    return lax.dot_general(
        sel, values, (((0,), (0,)), ((), ())), preferred_element_type=F32
    ).astype(BF)


def pick_far_body(ranks, chosen, tokens, keep, give, table, cols, sems):
    rows, width = cols.shape
    at = pl.multiple_of(lax.axis_index("tp") * width, width)
    one = pltpu.make_async_copy(chosen, table, sems.at[0])
    two = pltpu.make_async_copy(tokens.at[:, pl.ds(at, width)], cols, sems.at[1])
    one.start()
    two.start()
    one.wait()
    hit = hits(table, ranks, rows)
    two.wait()
    got = select(hit, cols[...])
    half = keep.shape[0]
    keep[...] = got[:half]
    give[...] = got[half:]


def pick_near_body(near, order, chosen, weights, tokens, keep, give, comb, tok, table, table_w, tok_v, sems):
    copies = (
        pltpu.make_async_copy(chosen, table, sems.at[0]),
        pltpu.make_async_copy(weights, table_w, sems.at[1]),
        pltpu.make_async_copy(tokens, tok_v, sems.at[2]),
    )
    for c in copies:
        c.start()
    copies[0].wait()
    copies[1].wait()
    rows = tok_v.shape[0]
    hit = hits(table, order, rows)
    w = table_row(table_w, order)
    high = w.astype(BF).astype(F32)
    n = hit.shape[1]
    comb[:, :n] = jnp.where(hit, high, 0.0).astype(BF)
    comb[:, n:] = jnp.where(hit, w - high, 0.0).astype(BF)
    sel = hits(table, near, rows)
    copies[2].wait()
    t = tok_v[...]
    tok[...] = t
    got = select(sel, t)
    half = keep.shape[0]
    keep[...] = got[:half]
    give[...] = got[half:]


def silu(v):
    return v / (1.0 + jnp.exp(-v))


def dense_in_body(tokens, w_in, w_gate, hidden, gate):
    t = tokens[...]
    hidden[...] = silu(dot(t, w_in[...])).astype(BF)
    g = jnp.sum(t.astype(F32) * w_gate[...].astype(F32), axis=1, keepdims=True)
    gate[...] = jax.nn.sigmoid(g)


def down(hidden, w_down, outs):
    tp = lax.axis_index("tp")
    width = outs[0].shape[1]
    for j in (3, 1, 2, 0):
        cols = pl.ds(pl.multiple_of((tp ^ j) * width, width), width)
        outs[j][...] = dot(hidden, w_down[:, cols]).astype(BF)


def near_body(a, b, c, w_gate, w_up, w_down, v_gate, v_up, v_down, p0, p1, p2, p3, sems):
    tiles = sems.shape[1]
    copies = []
    for i, (src, dst) in enumerate(((w_gate, v_gate), (w_up, v_up), (w_down, v_down))):
        size = src.shape[0] // tiles
        copies.append(
            [
                pltpu.make_async_copy(
                    src.at[pl.ds(size * k, size), :], dst.at[pl.ds(size * k, size), :], sems.at[i, k]
                )
                for k in range(tiles)
            ]
        )
    for k in range(tiles):
        copies[0][k].start()
        copies[1][k].start()
    for k in range(tiles):
        copies[2][k].start()
    x = jnp.concatenate([a[...], b[...], c[...]], axis=0)
    gate = up = 0.0
    size = v_gate.shape[0] // tiles
    for k in range(tiles):
        v = x[:, size * k : size * (k + 1)]
        copies[0][k].wait()
        gate = gate + dot(v, v_gate[pl.ds(size * k, size), :])
        copies[1][k].wait()
        up = up + dot(v, v_up[pl.ds(size * k, size), :])
    hidden = (silu(gate) * up).astype(BF)
    for k in range(tiles):
        copies[2][k].wait()
    down(hidden, v_down, (p0, p1, p2, p3))


def far_body(c0, c1, c2, c3, w_gate, w_up, w_down, p0, p1, p2, p3):
    tp = lax.axis_index("tp")
    width = c0.shape[1]
    gate = up = 0.0
    for j, chunk in enumerate((c0, c1, c2, c3)):
        at = pl.ds(pl.multiple_of((tp ^ j) * width, width), width)
        v = chunk[...]
        gate = gate + dot(v, w_gate[at, :])
        up = up + dot(v, w_up[at, :])
    hidden = (silu(gate) * up).astype(BF)
    down(hidden, w_down, (p0, p1, p2, p3))


def dense_out_body(h0, h1, h2, h3, w_out, gate, val):
    tp = lax.axis_index("tp")
    width = h0.shape[1]
    total = 0.0
    for j, h in enumerate((h0, h1, h2, h3)):
        rows = pl.ds(pl.multiple_of((tp ^ j) * width, width), width)
        total = total + dot(h[...], w_out[rows, :])
    val[...] = gate[...] * total


def combine_body(own, other, comb, val, out):
    half = own.shape[0]
    n = 2 * half
    a, b = own[...], other[...]
    total = val[...]
    for base in (0, n):
        total = total + dot(comb[:, base : base + half], a)
        total = total + dot(comb[:, base + half : base + n], b)
    out[...] = total.astype(BF)


def swap(v, axis, k):
    return lax.ppermute(v, axis, [(i, i ^ k) for i in range(lax.axis_size(axis))])


def fast(
    tokens,
    gate_proj,
    up_proj,
    down_proj,
    side_input_weight,
    dense_out,
    dense_gate,
    chosen_rows,
    choice_weights,
):
    experts, slots = chosen_rows.shape
    rows, model = tokens.shape
    width = model // lax.axis_size("tp")
    zs = experts // 2
    w_gate, w_up, w_down = gate_proj[0], up_proj[0], down_proj[0]
    order = tuple(range(0, experts, 2)) + tuple(range(1, experts, 2))
    near = (0, 2, 1, 3)
    far = tuple(range(4, experts, 2)) + tuple(range(5, experts, 2))
    fk = zs - 2
    dma = pltpu.SemaphoreType.DMA

    keep_f, give_f = pl.pallas_call(
        functools.partial(pick_far_body, far),
        out_shape=(shape((fk * slots, width), BF),) * 2,
        in_specs=[hbm(), hbm()],
        out_specs=(vmem(), vmem()),
        scratch_shapes=[
            pltpu.VMEM((experts, slots), jnp.int32),
            pltpu.VMEM((rows, width), BF),
            dma((2,)),
        ],
        compiler_params=pltpu.CompilerParams(vmem_limit_bytes=8 << 20),
        name="pick_far",
    )(*in_hbm(chosen_rows, tokens))
    got_f = swap(give_f, "ep", 1)
    keep_n, give_n, comb, tok = pl.pallas_call(
        functools.partial(pick_near_body, near, order),
        out_shape=(
            shape((2 * slots, model), BF),
            shape((2 * slots, model), BF),
            shape((rows, 2 * experts * slots), BF),
            shape((rows, model), BF),
        ),
        in_specs=[hbm()] * 3,
        out_specs=(vmem(),) * 4,
        scratch_shapes=[
            pltpu.VMEM((experts, slots), jnp.int32),
            pltpu.VMEM((experts, slots), F32),
            pltpu.VMEM((rows, model), BF),
            dma((3,)),
        ],
        compiler_params=pltpu.CompilerParams(vmem_limit_bytes=12 << 20),
        name="pick_near",
    )(*in_hbm(chosen_rows, choice_weights, tokens))
    got_n = swap(give_n, "ep", 1)

    zf = []
    for k in range(zs - 1, 1, -1):
        at = (k - 2) * slots
        block = jnp.concatenate([keep_f[at : at + slots], got_f[at : at + slots]], axis=0)
        zf.append(swap(block, "ep", 2 * k))
    z1 = swap(jnp.concatenate([keep_n[slots:], got_n[slots:]], axis=0), "ep", 2)

    hidden_own, side_gate = call(
        dense_in_body, (shape((rows, side_input_weight.shape[1]), BF), shape((rows, 1), F32)), 8
    )(tok, side_input_weight, dense_gate.reshape(1, model))
    hiddens = [hidden_own] + [swap(hidden_own, "tp", j) for j in (1, 2, 3)]

    arrived = jnp.concatenate(zf, axis=0)
    chunks = [arrived] + [swap(arrived, "tp", j) for j in (1, 2, 3)]

    v_gate, v_up, v_down, *near_part = pl.pallas_call(
        near_body,
        out_shape=(
            pltpu.VMEM(w_gate.shape, BF),
            pltpu.VMEM(w_up.shape, BF),
            pltpu.VMEM(w_down.shape, BF),
        )
        + (shape((4 * slots, width), BF),) * 4,
        in_specs=[vmem()] * 3 + [hbm()] * 3,
        out_specs=(vmem(),) * 7,
        scratch_shapes=[dma((3, 4))],
        compiler_params=pltpu.CompilerParams(vmem_limit_bytes=24 << 20),
        name="near",
    )(
        keep_n[:slots],
        got_n[:slots],
        z1,
        *in_hbm(w_gate, w_up, w_down),
    )
    far_part = call(far_body, (shape((2 * fk * slots, width), BF),) * 4, 24)(
        *chunks, v_gate, v_up, v_down
    )

    def reduce(part):
        sent = {j: swap(part[j], "tp", j) for j in (3, 1, 2)}
        total = part[0].astype(F32) + sent[1].astype(F32)
        return (total + sent[2].astype(F32) + sent[3].astype(F32)).astype(BF)

    sum_f = reduce(far_part)
    back = {}
    for i, k in enumerate(range(zs - 1, 1, -1)):
        back[k] = swap(sum_f[2 * slots * i : 2 * slots * (i + 1)], "ep", 2 * k)
    sum_n = reduce(near_part)
    back[0] = sum_n[: 2 * slots]
    back[1] = swap(sum_n[2 * slots :], "ep", 2)
    mine = jnp.concatenate([back[k][:slots] for k in range(zs)], axis=0)
    theirs = swap(jnp.concatenate([back[k][slots:] for k in range(zs)], axis=0), "ep", 1)

    val = call(dense_out_body, shape((rows, width), F32), 8)(*hiddens, dense_out, side_gate)
    return call(combine_body, shape((rows, width), BF), 8)(mine, theirs, comb, val)


def general(
    tokens,
    gate_proj,
    up_proj,
    down_proj,
    side_input_weight,
    dense_out,
    dense_gate,
    chosen_rows,
    choice_weights,
):
    tok_rows = tokens.shape[0]
    width = tokens.shape[1] // lax.axis_size("tp")
    column_position = lax.axis_index("tp") * width
    own_cols = lax.dynamic_slice_in_dim(tokens, column_position, width, 1)
    expert_count, slot_rows = chosen_rows.shape
    capacity = expert_count * slot_rows
    picked = jnp.take(own_cols, chosen_rows.reshape(-1), axis=0).reshape(
        expert_count, slot_rows, width
    )
    arrived = lax.all_to_all(picked, "ep", split_axis=0, concat_axis=1, tiled=True).reshape(
        capacity, width
    )
    w_gate = gate_proj[0]
    w_up = up_proj[0]
    w_down = down_proj[0]
    piece = lax.all_gather(arrived, "tp", axis=1, tiled=True)
    gate_val = jnp.dot(piece, w_gate, preferred_element_type=jnp.float32)
    up_val = jnp.dot(piece, w_up, preferred_element_type=jnp.float32)
    hidden = (jax.nn.silu(gate_val) * up_val).astype(jnp.bfloat16)
    summed = lax.psum_scatter(
        lax.dot_general(
            w_down, hidden, (((0,), (1,)), ((), ())), preferred_element_type=jnp.float32
        ).astype(jnp.bfloat16),
        "tp",
        scatter_dimension=0,
        tiled=True,
    )
    returned = lax.all_to_all(summed, "ep", split_axis=1, concat_axis=1, tiled=True)
    hits = (
        chosen_rows.reshape(-1)[:, None] == jnp.arange(tok_rows, dtype=jnp.int32)[None, :]
    ).astype(jnp.bfloat16)
    scaled = returned.astype(jnp.float32) * choice_weights.reshape(-1)[None, :]
    high_part = scaled.astype(jnp.bfloat16)
    lower_half = (scaled - high_part.astype(jnp.float32)).astype(jnp.bfloat16)
    contract = (((0,), (1,)), ((), ()))
    routed = lax.dot_general(
        hits, high_part, contract, preferred_element_type=jnp.float32
    ) + lax.dot_general(hits, lower_half, contract, preferred_element_type=jnp.float32)
    dense_hidden = jax.nn.silu(
        jnp.dot(tokens, side_input_weight, preferred_element_type=jnp.float32)
    ).astype(jnp.bfloat16)
    dense_val = jnp.dot(
        lax.all_gather(dense_hidden, "tp", axis=1, tiled=True),
        dense_out,
        preferred_element_type=jnp.float32,
    )
    side_gate = jax.nn.sigmoid(jnp.dot(tokens, dense_gate, preferred_element_type=jnp.float32))
    return (routed + side_gate[:, None] * dense_val).astype(jnp.bfloat16)


def per_device(tokens, gate_proj, *rest):
    experts = lax.axis_size("ep")
    fits = (
        lax.axis_size("tp") == 4
        and experts >= 4
        and experts & (experts - 1) == 0
        and tokens.shape[1] % (4 * 128) == 0
        and gate_proj.shape[2] % 128 == 0
        and rest[2].shape[1] % 128 == 0
        and tokens.shape[0] <= 512
        and rest[5].size <= 512
    )
    if not fits:
        return general(tokens, gate_proj, *rest)
    return fast(tokens, gate_proj, *rest)


def solution(mesh):
    placed = (
        P("ep", None),
        P("ep", None, "tp"),
        P("ep", None, "tp"),
        P("ep", "tp", None),
        P(None, "tp"),
        P(None, "tp"),
        P(),
        P(None, "ep"),
        P(None, "ep"),
    )
    return jax.shard_map(
        per_device, mesh=mesh, in_specs=placed, out_specs=P("ep", "tp"), check_vma=False
    )
```

```python
import functools

import jax
import jax.numpy as jnp
from jax import lax
from jax.experimental import pallas as pl
from jax.experimental.pallas import tpu as pltpu
from jax.sharding import PartitionSpec as P

BF = jnp.bfloat16
F32 = jnp.float32


COST = pl.CostEstimate(flops=8_000_000_000, bytes_accessed=1 << 20, transcendentals=0)


def call(body, outs, limit_mib, cost=None):
    return pl.pallas_call(
        body,
        out_shape=outs,
        cost_estimate=cost,
        compiler_params=pltpu.CompilerParams(vmem_limit_bytes=limit_mib << 20),
    )


def shape(dims, dtype):
    return jax.ShapeDtypeStruct(dims, dtype)


def dot(a, b):
    return jnp.dot(a, b, preferred_element_type=F32)


def hbm():
    return pl.BlockSpec(memory_space=pltpu.HBM)


def in_hbm(*arrays):
    return [pltpu.with_memory_space_constraint(a, pltpu.HBM) for a in arrays]


def vmem():
    return pl.BlockSpec(memory_space=pltpu.VMEM)


def table_row(table, ranks):
    me = lax.axis_index("ep")
    return jnp.concatenate([table[pl.ds(me ^ r, 1), :] for r in ranks], axis=1)


def hits(table, ranks, rows):
    slots = table_row(table, ranks)
    return lax.broadcasted_iota(jnp.int32, (rows, slots.shape[1]), 0) == slots


def select(hit, values):
    sel = jnp.where(hit, 1.0, 0.0).astype(BF)
    return lax.dot_general(
        sel, values, (((0,), (0,)), ((), ())), preferred_element_type=F32
    ).astype(BF)


def pick_far_body(ranks, chosen, tokens, keep, give, table, cols, sems):
    rows = cols.shape[0]
    width = cols.shape[1] // 2
    copies = [pltpu.make_async_copy(chosen, table, sems.at[0])]
    for i, j in enumerate((0, 3)):
        copies.append(
            pltpu.make_async_copy(
                tokens.at[:, block(j, width)], cols.at[:, pl.ds(width * i, width)], sems.at[1 + i]
            )
        )
    for c in copies:
        c.start()
    copies[0].wait()
    hit = hits(table, ranks, rows)
    for c in copies[1:]:
        c.wait()
    got = select(hit, cols[...])
    half = keep.shape[0]
    keep[...] = got[:half]
    give[...] = got[half:]


def pick_near_body(near, order, chosen, weights, tokens, keep, give, next_a, next_b, comb):
    rows = tokens.shape[0]
    got = select(hits(chosen, near, rows), tokens[...])
    size = keep.shape[0]
    for i, out in enumerate((keep, give, next_a, next_b)):
        out[...] = got[size * i : size * (i + 1)]
    hit = hits(chosen, order, rows)
    w = table_row(weights, order)
    high = w.astype(BF).astype(F32)
    n = hit.shape[1]
    comb[:, :n] = jnp.where(hit, high, 0.0).astype(BF)
    comb[:, n:] = jnp.where(hit, w - high, 0.0).astype(BF)


def silu(v):
    return v / (1.0 + jnp.exp(-v))


def dense_in_body(tokens, w_in, w_gate, hidden, gate):
    t = tokens[...]
    hidden[...] = silu(dot(t, w_in[...])).astype(BF)
    w = w_gate[...].astype(F32)[None, :]
    g = jnp.sum(t.astype(F32) * w, axis=1, keepdims=True)
    gate[...] = jax.nn.sigmoid(g)


def block(j, width):
    return pl.ds(pl.multiple_of((lax.axis_index("tp") ^ j) * width, width), width)


def down(hidden, w_down, outs):
    for j, out in outs:
        out[...] = dot(hidden, w_down[:, block(j, out.shape[1])]).astype(BF)


def enter(chunks, w_gate, w_up):
    gate = up = 0.0
    for j, chunk in chunks:
        v = chunk[...]
        at = block(j, v.shape[1])
        gate = gate + dot(v, w_gate[at, :])
        up = up + dot(v, w_up[at, :])
    return gate, up


def near_body(a, b, c, d, w_gate, w_up, w_down, p0, p1, p2, p3):
    x = jnp.concatenate([a[...], b[...], c[...], d[...]], axis=0)
    gate, up = dot(x, w_gate[...]), dot(x, w_up[...])
    down((silu(gate) * up).astype(BF), w_down, ((3, p3), (1, p1), (2, p2), (0, p0)))


def far_a_body(c0, c1, w_gate, w_up, w_down, acc_gate, acc_up):
    del w_down
    acc_gate[...], acc_up[...] = enter(((0, c0), (1, c1)), w_gate, w_up)


def far_b_body(c2, c3, acc_gate, acc_up, w_gate, w_up, w_down, hidden, p3):
    gate, up = enter(((2, c2), (3, c3)), w_gate, w_up)
    gate, up = gate + acc_gate[...], up + acc_up[...]
    h = (silu(gate) * up).astype(BF)
    hidden[...] = h
    down(h, w_down, ((3, p3),))


def far_c_body(hidden, w_down, p0, p1, p2):
    down(hidden[...], w_down, ((1, p1), (2, p2), (0, p0)))


def dense_out_body(h0, h1, h2, h3, w_out, gate, val):
    total = 0.0
    for j, h in enumerate((h0, h1, h2, h3)):
        total = total + dot(h[...], w_out[block(j, h.shape[1]), :])
    val[...] = gate[...] * total


def combine_body(own, other, comb, val, out):
    x = jnp.concatenate([own[...], other[...]], axis=0)
    n = x.shape[0]
    out[...] = (val[...] + dot(comb[:, :n], x) + dot(comb[:, n:], x)).astype(BF)


def exchange(values):
    got = {0: values[0]}
    for j in (3, 1, 2):
        if j < len(values):
            got[j] = swap(values[j], "tp", j)
    return [got[j] for j in range(len(values))]


def swap(v, axis, k):
    return lax.ppermute(v, axis, [(i, i ^ k) for i in range(lax.axis_size(axis))])


def fast(
    tokens,
    gate_proj,
    up_proj,
    down_proj,
    side_input_weight,
    dense_out,
    dense_gate,
    chosen_rows,
    choice_weights,
):
    experts, slots = chosen_rows.shape
    rows, model = tokens.shape
    width = model // lax.axis_size("tp")
    zs = experts // 2
    w_gate, w_up, w_down = gate_proj[0], up_proj[0], down_proj[0]
    ff = w_gate.shape[1]
    near = (0, 1, 2, 3)
    order = tuple(range(0, experts, 2)) + tuple(range(1, experts, 2))
    far = tuple(range(4, experts, 2)) + tuple(range(5, experts, 2))
    fk = zs - 2
    dma = pltpu.SemaphoreType.DMA

    keep_f, give_f = pl.pallas_call(
        functools.partial(pick_far_body, far),
        out_shape=(shape((fk * slots, 2 * width), BF),) * 2,
        in_specs=[hbm(), hbm()],
        out_specs=(vmem(), vmem()),
        scratch_shapes=[
            pltpu.VMEM((experts, slots), jnp.int32),
            pltpu.VMEM((rows, 2 * width), BF),
            dma((3,)),
        ],
        compiler_params=pltpu.CompilerParams(vmem_limit_bytes=8 << 20),
        cost_estimate=COST,
        name="pick_far",
    )(*in_hbm(chosen_rows, tokens))
    got_f = swap(give_f, "ep", 1)
    keep_n, give_n, next_a, next_b, comb = call(
        functools.partial(pick_near_body, near, order),
        (shape((slots, model), BF),) * 4
        + (shape((rows, 2 * experts * slots), BF),),
        8,
        COST,
    )(chosen_rows, choice_weights, tokens)
    got_n = swap(give_n, "ep", 1)
    z1a = swap(next_a, "ep", 2)
    z1b = swap(next_b, "ep", 3)

    waves = []
    for cols in (slice(0, width), slice(width, 2 * width)):
        got = []
        for k in range(zs - 1, 1, -1):
            at = (k - 2) * slots
            rows_k = jnp.concatenate([keep_f[at : at + slots, cols], got_f[at : at + slots, cols]])
            got.append(swap(rows_k, "ep", 2 * k))
        waves.append(jnp.concatenate(got, axis=0))

    hidden_own, side_gate = call(
        dense_in_body,
        (shape((rows, side_input_weight.shape[1]), BF), shape((rows, 1), F32)),
        8,
        COST,
    )(tokens, side_input_weight, dense_gate)
    hiddens = exchange([hidden_own] * 4)

    chunks = exchange([waves[0]] * 3)

    near_part = call(near_body, (shape((4 * slots, width), BF),) * 4, 8)(
        keep_n, got_n, z1a, z1b, w_gate, w_up, w_down
    )
    far_rows = 2 * fk * slots
    accs = call(far_a_body, (shape((far_rows, ff), F32),) * 2, 8)(
        chunks[0], chunks[1], w_gate, w_up, w_down
    )
    hidden, part3 = call(
        far_b_body, (shape((far_rows, ff), BF), shape((far_rows, width), BF)), 8
    )(chunks[2], waves[1], *accs, w_gate, w_up, w_down)
    far_part = call(far_c_body, (shape((far_rows, width), BF),) * 3, 8)(hidden, w_down)
    far_part = [*far_part, part3]

    def reduce(part):
        sent = exchange(part)
        total = part[0].astype(F32) + sent[1].astype(F32)
        return (total + sent[2].astype(F32) + sent[3].astype(F32)).astype(BF)

    sum_f = reduce(far_part)
    back = {}
    for i, k in enumerate(range(zs - 1, 1, -1)):
        back[k] = swap(sum_f[2 * slots * i : 2 * slots * (i + 1)], "ep", 2 * k)
    sum_n = reduce(near_part)
    back[0] = sum_n[: 2 * slots]
    back[1] = swap(sum_n[2 * slots :], "ep", 2)
    mine = jnp.concatenate([back[k][:slots] for k in range(zs)], axis=0)
    theirs = swap(jnp.concatenate([back[k][slots:] for k in range(zs)], axis=0), "ep", 1)

    val = call(dense_out_body, shape((rows, width), F32), 8)(*hiddens, dense_out, side_gate)
    return call(combine_body, shape((rows, width), BF), 8)(mine, theirs, comb, val)


def general(
    tokens,
    gate_proj,
    up_proj,
    down_proj,
    side_input_weight,
    dense_out,
    dense_gate,
    chosen_rows,
    choice_weights,
):
    tok_rows = tokens.shape[0]
    width = tokens.shape[1] // lax.axis_size("tp")
    column_position = lax.axis_index("tp") * width
    own_cols = lax.dynamic_slice_in_dim(tokens, column_position, width, 1)
    expert_count, slot_rows = chosen_rows.shape
    capacity = expert_count * slot_rows
    picked = jnp.take(own_cols, chosen_rows.reshape(-1), axis=0).reshape(
        expert_count, slot_rows, width
    )
    arrived = lax.all_to_all(picked, "ep", split_axis=0, concat_axis=1, tiled=True).reshape(
        capacity, width
    )
    w_gate = gate_proj[0]
    w_up = up_proj[0]
    w_down = down_proj[0]
    piece = lax.all_gather(arrived, "tp", axis=1, tiled=True)
    gate_val = jnp.dot(piece, w_gate, preferred_element_type=jnp.float32)
    up_val = jnp.dot(piece, w_up, preferred_element_type=jnp.float32)
    hidden = (jax.nn.silu(gate_val) * up_val).astype(jnp.bfloat16)
    summed = lax.psum_scatter(
        lax.dot_general(
            w_down, hidden, (((0,), (1,)), ((), ())), preferred_element_type=jnp.float32
        ).astype(jnp.bfloat16),
        "tp",
        scatter_dimension=0,
        tiled=True,
    )
    returned = lax.all_to_all(summed, "ep", split_axis=1, concat_axis=1, tiled=True)
    hits = (
        chosen_rows.reshape(-1)[:, None] == jnp.arange(tok_rows, dtype=jnp.int32)[None, :]
    ).astype(jnp.bfloat16)
    scaled = returned.astype(jnp.float32) * choice_weights.reshape(-1)[None, :]
    high_part = scaled.astype(jnp.bfloat16)
    lower_half = (scaled - high_part.astype(jnp.float32)).astype(jnp.bfloat16)
    contract = (((0,), (1,)), ((), ()))
    routed = lax.dot_general(
        hits, high_part, contract, preferred_element_type=jnp.float32
    ) + lax.dot_general(hits, lower_half, contract, preferred_element_type=jnp.float32)
    dense_hidden = jax.nn.silu(
        jnp.dot(tokens, side_input_weight, preferred_element_type=jnp.float32)
    ).astype(jnp.bfloat16)
    dense_val = jnp.dot(
        lax.all_gather(dense_hidden, "tp", axis=1, tiled=True),
        dense_out,
        preferred_element_type=jnp.float32,
    )
    side_gate = jax.nn.sigmoid(jnp.dot(tokens, dense_gate, preferred_element_type=jnp.float32))
    return (routed + side_gate[:, None] * dense_val).astype(jnp.bfloat16)


def per_device(tokens, gate_proj, *rest):
    experts = lax.axis_size("ep")
    fits = (
        lax.axis_size("tp") == 4
        and experts >= 8
        and experts & (experts - 1) == 0
        and tokens.shape[1] % (4 * 128) == 0
        and gate_proj.shape[2] % 128 == 0
        and rest[2].shape[1] % 128 == 0
        and tokens.shape[0] <= 512
        and rest[5].size <= 512
    )
    if not fits:
        return general(tokens, gate_proj, *rest)
    return fast(tokens, gate_proj, *rest)


def solution(mesh):
    placed = (
        P("ep", None),
        P("ep", None, "tp"),
        P("ep", None, "tp"),
        P("ep", "tp", None),
        P(None, "tp"),
        P(None, "tp"),
        P(),
        P(None, "ep"),
        P(None, "ep"),
    )
    return jax.shard_map(
        per_device, mesh=mesh, in_specs=placed, out_specs=P("ep", "tp"), check_vma=False
    )
```

```python
import functools

import jax
import jax.numpy as jnp
from jax import lax
from jax.experimental import pallas as pl
from jax.experimental.pallas import tpu as pltpu
from jax.sharding import PartitionSpec as P

BF = jnp.bfloat16
F32 = jnp.float32


COST = pl.CostEstimate(flops=8_000_000_000, bytes_accessed=1 << 20, transcendentals=0)


def call(body, outs, limit_mib, cost=None):
    return pl.pallas_call(
        body,
        out_shape=outs,
        cost_estimate=cost,
        compiler_params=pltpu.CompilerParams(vmem_limit_bytes=limit_mib << 20),
    )


def shape(dims, dtype):
    return jax.ShapeDtypeStruct(dims, dtype)


def dot(a, b):
    return jnp.dot(a, b, preferred_element_type=F32)


def hbm():
    return pl.BlockSpec(memory_space=pltpu.HBM)


def in_hbm(*arrays):
    return [pltpu.with_memory_space_constraint(a, pltpu.HBM) for a in arrays]


def vmem():
    return pl.BlockSpec(memory_space=pltpu.VMEM)


def table_row(table, ranks):
    me = lax.axis_index("ep")
    return jnp.concatenate([table[pl.ds(me ^ r, 1), :] for r in ranks], axis=1)


def hits(table, ranks, rows):
    slots = table_row(table, ranks)
    return lax.broadcasted_iota(jnp.int32, (rows, slots.shape[1]), 0) == slots


def select(hit, values):
    sel = jnp.where(hit, 1.0, 0.0).astype(BF)
    return lax.dot_general(
        sel, values, (((0,), (0,)), ((), ())), preferred_element_type=F32
    ).astype(BF)


def pick_far_body(ranks, chosen, tokens, keep, give, table, cols, sems):
    rows = cols.shape[0]
    width = cols.shape[1] // 2
    copies = [pltpu.make_async_copy(chosen, table, sems.at[0])]
    for i, j in enumerate((0, 3)):
        copies.append(
            pltpu.make_async_copy(
                tokens.at[:, block(j, width)], cols.at[:, pl.ds(width * i, width)], sems.at[1 + i]
            )
        )
    for c in copies:
        c.start()
    copies[0].wait()
    hit = hits(table, ranks, rows)
    for c in copies[1:]:
        c.wait()
    got = select(hit, cols[...])
    half = keep.shape[0]
    keep[...] = got[:half]
    give[...] = got[half:]


def pick_near_body(near, order, chosen, weights, tokens, keep, give, next_a, next_b, comb):
    rows = tokens.shape[0]
    got = select(hits(chosen, near, rows), tokens[...])
    size = keep.shape[0]
    for i, out in enumerate((keep, give, next_a, next_b)):
        out[...] = got[size * i : size * (i + 1)]
    hit = hits(chosen, order, rows)
    w = table_row(weights, order)
    high = w.astype(BF).astype(F32)
    n = hit.shape[1]
    comb[:, :n] = jnp.where(hit, high, 0.0).astype(BF)
    comb[:, n:] = jnp.where(hit, w - high, 0.0).astype(BF)


def silu(v):
    return v / (1.0 + jnp.exp(-v))


def dense_in_body(tokens, w_in, w_gate, hidden, gate):
    t = tokens[...]
    hidden[...] = silu(dot(t, w_in[...])).astype(BF)
    w = w_gate[...].astype(F32)[None, :]
    g = jnp.sum(t.astype(F32) * w, axis=1, keepdims=True)
    gate[...] = jax.nn.sigmoid(g)


def block(j, width):
    return pl.ds(pl.multiple_of((lax.axis_index("tp") ^ j) * width, width), width)


def down(hidden, w_down, outs):
    for j, out in outs:
        out[...] = dot(hidden, w_down[:, block(j, out.shape[1])]).astype(BF)


def enter(chunks, w_gate, w_up):
    gate = up = 0.0
    for j, chunk in chunks:
        v = chunk[...]
        at = block(j, v.shape[1])
        gate = gate + dot(v, w_gate[at, :])
        up = up + dot(v, w_up[at, :])
    return gate, up


def near_body(a, b, c, d, w_gate, w_up, w_down, p0, p1, p2, p3):
    x = jnp.concatenate([a[...], b[...], c[...], d[...]], axis=0)
    gate, up = dot(x, w_gate[...]), dot(x, w_up[...])
    down((silu(gate) * up).astype(BF), w_down, ((3, p3), (1, p1), (2, p2), (0, p0)))


def far_a_body(c0, c1, w_gate, w_up, w_down, acc_gate, acc_up):
    del w_down
    acc_gate[...], acc_up[...] = enter(((0, c0), (1, c1)), w_gate, w_up)


def far_b_body(c2, c3, acc_gate, acc_up, w_gate, w_up, w_down, hidden, p3):
    gate, up = enter(((2, c2), (3, c3)), w_gate, w_up)
    gate, up = gate + acc_gate[...], up + acc_up[...]
    h = (silu(gate) * up).astype(BF)
    hidden[...] = h
    down(h, w_down, ((3, p3),))


def far_c_body(hidden, w_down, p0, p1, p2):
    down(hidden[...], w_down, ((1, p1), (2, p2), (0, p0)))


def dense_out_body(h0, h1, h2, h3, w_out, gate, val):
    total = 0.0
    for j, h in enumerate((h0, h1, h2, h3)):
        total = total + dot(h[...], w_out[block(j, h.shape[1]), :])
    val[...] = gate[...] * total


def combine_body(own, next_own, other, next_other, comb, val, out):
    x = jnp.concatenate([r[...] for r in (own, next_own, other, next_other)], axis=0)
    n = x.shape[0]
    out[...] = (val[...] + dot(comb[:, :n], x) + dot(comb[:, n:], x)).astype(BF)


def exchange(values):
    got = {0: values[0]}
    for j in (3, 1, 2):
        if j < len(values):
            got[j] = swap(values[j], "tp", j)
    return [got[j] for j in range(len(values))]


def swap(v, axis, k):
    return lax.ppermute(v, axis, [(i, i ^ k) for i in range(lax.axis_size(axis))])


def fast(
    tokens,
    gate_proj,
    up_proj,
    down_proj,
    side_input_weight,
    dense_out,
    dense_gate,
    chosen_rows,
    choice_weights,
):
    experts, slots = chosen_rows.shape
    rows, model = tokens.shape
    width = model // lax.axis_size("tp")
    zs = experts // 2
    w_gate, w_up, w_down = gate_proj[0], up_proj[0], down_proj[0]
    ff = w_gate.shape[1]
    near = (0, 1, 2, 3)
    own = (0, *range(4, experts, 2), 2)
    order = own + tuple(r + 1 for r in own)
    far = tuple(range(4, experts, 2)) + tuple(range(5, experts, 2))
    fk = zs - 2
    dma = pltpu.SemaphoreType.DMA

    keep_f, give_f = pl.pallas_call(
        functools.partial(pick_far_body, far),
        out_shape=(shape((fk * slots, 2 * width), BF),) * 2,
        in_specs=[hbm(), hbm()],
        out_specs=(vmem(), vmem()),
        scratch_shapes=[
            pltpu.VMEM((experts, slots), jnp.int32),
            pltpu.VMEM((rows, 2 * width), BF),
            dma((3,)),
        ],
        compiler_params=pltpu.CompilerParams(vmem_limit_bytes=8 << 20),
        cost_estimate=COST,
        name="pick_far",
    )(*in_hbm(chosen_rows, tokens))
    got_f = swap(give_f, "ep", 1)
    keep_n, give_n, next_a, next_b, comb = call(
        functools.partial(pick_near_body, near, order),
        (shape((slots, model), BF),) * 4
        + (shape((rows, 2 * experts * slots), BF),),
        8,
        COST,
    )(chosen_rows, choice_weights, tokens)
    got_n = swap(give_n, "ep", 1)
    z1a = swap(next_a, "ep", 2)
    z1b = swap(next_b, "ep", 3)

    waves = []
    for cols in (slice(0, width), slice(width, 2 * width)):
        got = []
        for k in range(zs - 1, 1, -1):
            at = (k - 2) * slots
            rows_k = jnp.concatenate([keep_f[at : at + slots, cols], got_f[at : at + slots, cols]])
            got.append(swap(rows_k, "ep", 2 * k))
        waves.append(jnp.concatenate(got, axis=0))

    hidden_own, side_gate = call(
        dense_in_body,
        (shape((rows, side_input_weight.shape[1]), BF), shape((rows, 1), F32)),
        8,
        COST,
    )(tokens, side_input_weight, dense_gate)
    hiddens = exchange([hidden_own] * 4)

    chunks = exchange([waves[0]] * 3)

    near_part = call(near_body, (shape((4 * slots, width), BF),) * 4, 8)(
        keep_n, got_n, z1a, z1b, w_gate, w_up, w_down
    )
    far_rows = 2 * fk * slots
    accs = call(far_a_body, (shape((far_rows, ff), F32),) * 2, 8)(
        chunks[0], chunks[1], w_gate, w_up, w_down
    )
    hidden, part3 = call(
        far_b_body, (shape((far_rows, ff), BF), shape((far_rows, width), BF)), 8
    )(chunks[2], waves[1], *accs, w_gate, w_up, w_down)
    far_part = call(far_c_body, (shape((far_rows, width), BF),) * 3, 8)(hidden, w_down)
    far_part = [*far_part, part3]

    def reduce(part):
        sent = exchange(part)
        total = part[0].astype(F32) + sent[1].astype(F32)
        return (total + sent[2].astype(F32) + sent[3].astype(F32)).astype(BF)

    sum_f = reduce(far_part)
    back = {}
    for i, k in enumerate(range(zs - 1, 1, -1)):
        back[k] = swap(sum_f[2 * slots * i : 2 * slots * (i + 1)], "ep", 2 * k)
    sum_n = reduce(near_part)
    next_own, next_other = [], []
    for at, k, got in ((2, 2, next_own), (3, 3, next_other)):
        got.append(swap(sum_n[at * slots : (at + 1) * slots], "ep", k))
    parts = [sum_n[: 2 * slots]] + [back[k] for k in range(2, zs)]
    mine = jnp.concatenate([p[:slots] for p in parts], axis=0)
    theirs = swap(jnp.concatenate([p[slots:] for p in parts], axis=0), "ep", 1)

    val = call(dense_out_body, shape((rows, width), F32), 8)(*hiddens, dense_out, side_gate)
    return call(combine_body, shape((rows, width), BF), 8)(
        mine, *next_own, theirs, *next_other, comb, val
    )


def general(
    tokens,
    gate_proj,
    up_proj,
    down_proj,
    side_input_weight,
    dense_out,
    dense_gate,
    chosen_rows,
    choice_weights,
):
    tok_rows = tokens.shape[0]
    width = tokens.shape[1] // lax.axis_size("tp")
    column_position = lax.axis_index("tp") * width
    own_cols = lax.dynamic_slice_in_dim(tokens, column_position, width, 1)
    expert_count, slot_rows = chosen_rows.shape
    capacity = expert_count * slot_rows
    picked = jnp.take(own_cols, chosen_rows.reshape(-1), axis=0).reshape(
        expert_count, slot_rows, width
    )
    arrived = lax.all_to_all(picked, "ep", split_axis=0, concat_axis=1, tiled=True).reshape(
        capacity, width
    )
    w_gate = gate_proj[0]
    w_up = up_proj[0]
    w_down = down_proj[0]
    piece = lax.all_gather(arrived, "tp", axis=1, tiled=True)
    gate_val = jnp.dot(piece, w_gate, preferred_element_type=jnp.float32)
    up_val = jnp.dot(piece, w_up, preferred_element_type=jnp.float32)
    hidden = (jax.nn.silu(gate_val) * up_val).astype(jnp.bfloat16)
    summed = lax.psum_scatter(
        lax.dot_general(
            w_down, hidden, (((0,), (1,)), ((), ())), preferred_element_type=jnp.float32
        ).astype(jnp.bfloat16),
        "tp",
        scatter_dimension=0,
        tiled=True,
    )
    returned = lax.all_to_all(summed, "ep", split_axis=1, concat_axis=1, tiled=True)
    hits = (
        chosen_rows.reshape(-1)[:, None] == jnp.arange(tok_rows, dtype=jnp.int32)[None, :]
    ).astype(jnp.bfloat16)
    scaled = returned.astype(jnp.float32) * choice_weights.reshape(-1)[None, :]
    high_part = scaled.astype(jnp.bfloat16)
    lower_half = (scaled - high_part.astype(jnp.float32)).astype(jnp.bfloat16)
    contract = (((0,), (1,)), ((), ()))
    routed = lax.dot_general(
        hits, high_part, contract, preferred_element_type=jnp.float32
    ) + lax.dot_general(hits, lower_half, contract, preferred_element_type=jnp.float32)
    dense_hidden = jax.nn.silu(
        jnp.dot(tokens, side_input_weight, preferred_element_type=jnp.float32)
    ).astype(jnp.bfloat16)
    dense_val = jnp.dot(
        lax.all_gather(dense_hidden, "tp", axis=1, tiled=True),
        dense_out,
        preferred_element_type=jnp.float32,
    )
    side_gate = jax.nn.sigmoid(jnp.dot(tokens, dense_gate, preferred_element_type=jnp.float32))
    return (routed + side_gate[:, None] * dense_val).astype(jnp.bfloat16)


def per_device(tokens, gate_proj, *rest):
    experts = lax.axis_size("ep")
    fits = (
        lax.axis_size("tp") == 4
        and experts >= 8
        and experts & (experts - 1) == 0
        and tokens.shape[1] % (4 * 128) == 0
        and gate_proj.shape[2] % 128 == 0
        and rest[2].shape[1] % 128 == 0
        and tokens.shape[0] <= 512
        and rest[5].size <= 512
    )
    if not fits:
        return general(tokens, gate_proj, *rest)
    return fast(tokens, gate_proj, *rest)


def solution(mesh):
    placed = (
        P("ep", None),
        P("ep", None, "tp"),
        P("ep", None, "tp"),
        P("ep", "tp", None),
        P(None, "tp"),
        P(None, "tp"),
        P(),
        P(None, "ep"),
        P(None, "ep"),
    )
    return jax.shard_map(
        per_device, mesh=mesh, in_specs=placed, out_specs=P("ep", "tp"), check_vma=False
    )
```

```python
import functools

import jax
import jax.numpy as jnp
from jax import lax
from jax.experimental import pallas as pl
from jax.experimental.pallas import tpu as pltpu
from jax.sharding import PartitionSpec as P

BF = jnp.bfloat16
F32 = jnp.float32


COST = pl.CostEstimate(flops=8_000_000_000, bytes_accessed=1 << 20, transcendentals=0)


def call(body, outs, limit_mib, cost=None):
    return pl.pallas_call(
        body,
        out_shape=outs,
        cost_estimate=cost,
        compiler_params=pltpu.CompilerParams(vmem_limit_bytes=limit_mib << 20),
    )


def shape(dims, dtype):
    return jax.ShapeDtypeStruct(dims, dtype)


def dot(a, b):
    return jnp.dot(a, b, preferred_element_type=F32)


def hbm():
    return pl.BlockSpec(memory_space=pltpu.HBM)


def in_hbm(*arrays):
    return [pltpu.with_memory_space_constraint(a, pltpu.HBM) for a in arrays]


def vmem():
    return pl.BlockSpec(memory_space=pltpu.VMEM)


def table_row(table, ranks):
    me = lax.axis_index("ep")
    return jnp.concatenate([table[pl.ds(me ^ r, 1), :] for r in ranks], axis=1)


def hits(table, ranks, rows):
    slots = table_row(table, ranks)
    return lax.broadcasted_iota(jnp.int32, (rows, slots.shape[1]), 0) == slots


def select(hit, values):
    sel = jnp.where(hit, 1.0, 0.0).astype(BF)
    return lax.dot_general(
        sel, values, (((0,), (0,)), ((), ())), preferred_element_type=F32
    ).astype(BF)


def pick_far_body(ranks, chosen, tokens, keep, give, table, cols, sems):
    rows = cols.shape[0]
    width = cols.shape[1] // 2
    copies = [pltpu.make_async_copy(chosen, table, sems.at[0])]
    for i, j in enumerate((0, 3)):
        copies.append(
            pltpu.make_async_copy(
                tokens.at[:, block(j, width)], cols.at[:, pl.ds(width * i, width)], sems.at[1 + i]
            )
        )
    for c in copies:
        c.start()
    copies[0].wait()
    hit = hits(table, ranks, rows)
    for c in copies[1:]:
        c.wait()
    got = select(hit, cols[...])
    half = keep.shape[0]
    keep[...] = got[:half]
    give[...] = got[half:]


def pick_near_body(near, order, chosen, weights, tokens, keep, give, next_a, next_b, comb):
    rows = tokens.shape[0]
    got = select(hits(chosen, near, rows), tokens[...])
    size = keep.shape[0]
    for i, out in enumerate((keep, give, next_a, next_b)):
        out[...] = got[size * i : size * (i + 1)]
    hit = hits(chosen, order, rows)
    w = table_row(weights, order)
    high = w.astype(BF).astype(F32)
    n = hit.shape[1]
    comb[:, :n] = jnp.where(hit, high, 0.0).astype(BF)
    comb[:, n:] = jnp.where(hit, w - high, 0.0).astype(BF)


def silu(v):
    return v / (1.0 + jnp.exp(-v))


def dense_in_body(tokens, w_in, w_gate, hidden, gate):
    t = tokens[...]
    hidden[...] = silu(dot(t, w_in[...])).astype(BF)
    w = w_gate[...].astype(F32)[None, :]
    g = jnp.sum(t.astype(F32) * w, axis=1, keepdims=True)
    gate[...] = jax.nn.sigmoid(g)


def block(j, width):
    return pl.ds(pl.multiple_of((lax.axis_index("tp") ^ j) * width, width), width)


def down(hidden, w_down, outs):
    for j, out in outs:
        out[...] = dot(hidden, w_down[:, block(j, out.shape[1])]).astype(BF)


def enter(chunks, w_gate, w_up):
    gate = up = 0.0
    for j, chunk in chunks:
        v = chunk[...]
        at = block(j, v.shape[1])
        gate = gate + dot(v, w_gate[at, :])
        up = up + dot(v, w_up[at, :])
    return gate, up


def near_body(a, b, c, d, w_gate, w_up, w_down, p0, p1, p2, p3):
    x = jnp.concatenate([a[...], b[...], c[...], d[...]], axis=0)
    gate, up = dot(x, w_gate[...]), dot(x, w_up[...])
    down((silu(gate) * up).astype(BF), w_down, ((3, p3), (1, p1), (2, p2), (0, p0)))


def far_body(c0, c1, c2, c3, w_gate, w_up, w_down, p0, p1, p2, p3):
    gate, up = enter(((0, c0), (1, c1), (2, c2), (3, c3)), w_gate, w_up)
    h = (silu(gate) * up).astype(BF)
    down(h, w_down, ((3, p3), (1, p1), (2, p2), (0, p0)))


def dense_out_body(h0, h1, h2, h3, w_out, gate, val):
    total = 0.0
    for j, h in enumerate((h0, h1, h2, h3)):
        total = total + dot(h[...], w_out[block(j, h.shape[1]), :])
    val[...] = gate[...] * total


def combine_body(own, next_own, other, next_other, comb, val, out):
    x = jnp.concatenate([r[...] for r in (own, next_own, other, next_other)], axis=0)
    n = x.shape[0]
    out[...] = (val[...] + dot(comb[:, :n], x) + dot(comb[:, n:], x)).astype(BF)


def exchange(values):
    got = {0: values[0]}
    for j in (3, 1, 2):
        if j < len(values):
            got[j] = swap(values[j], "tp", j)
    return [got[j] for j in range(len(values))]


def swap(v, axis, k):
    return lax.ppermute(v, axis, [(i, i ^ k) for i in range(lax.axis_size(axis))])


def fast(
    tokens,
    gate_proj,
    up_proj,
    down_proj,
    side_input_weight,
    dense_out,
    dense_gate,
    chosen_rows,
    choice_weights,
):
    experts, slots = chosen_rows.shape
    rows, model = tokens.shape
    width = model // lax.axis_size("tp")
    zs = experts // 2
    w_gate, w_up, w_down = gate_proj[0], up_proj[0], down_proj[0]
    near = (0, 1, 2, 3)
    own = (0, *range(4, experts, 2), 2)
    order = own + tuple(r + 1 for r in own)
    far = tuple(range(4, experts, 2)) + tuple(range(5, experts, 2))
    fk = zs - 2
    dma = pltpu.SemaphoreType.DMA

    keep_f, give_f = pl.pallas_call(
        functools.partial(pick_far_body, far),
        out_shape=(shape((fk * slots, 2 * width), BF),) * 2,
        in_specs=[hbm(), hbm()],
        out_specs=(vmem(), vmem()),
        scratch_shapes=[
            pltpu.VMEM((experts, slots), jnp.int32),
            pltpu.VMEM((rows, 2 * width), BF),
            dma((3,)),
        ],
        compiler_params=pltpu.CompilerParams(vmem_limit_bytes=8 << 20),
        cost_estimate=COST,
        name="pick_far",
    )(*in_hbm(chosen_rows, tokens))
    got_f = swap(give_f, "ep", 1)
    keep_n, give_n, next_a, next_b, comb = call(
        functools.partial(pick_near_body, near, order),
        (shape((slots, model), BF),) * 4
        + (shape((rows, 2 * experts * slots), BF),),
        8,
        COST,
    )(chosen_rows, choice_weights, tokens)
    got_n = swap(give_n, "ep", 1)
    z1a = swap(next_a, "ep", 2)
    z1b = swap(next_b, "ep", 3)

    waves = []
    for cols in (slice(0, width), slice(width, 2 * width)):
        got = []
        for k in range(zs - 1, 1, -1):
            at = (k - 2) * slots
            rows_k = jnp.concatenate([keep_f[at : at + slots, cols], got_f[at : at + slots, cols]])
            got.append(swap(rows_k, "ep", 2 * k))
        waves.append(jnp.concatenate(got, axis=0))

    hidden_own, side_gate = call(
        dense_in_body,
        (shape((rows, side_input_weight.shape[1]), BF), shape((rows, 1), F32)),
        8,
        COST,
    )(tokens, side_input_weight, dense_gate)
    hiddens = exchange([hidden_own] * 4)

    chunks = exchange([waves[0]] * 3)

    near_part = call(near_body, (shape((4 * slots, width), BF),) * 4, 8)(
        keep_n, got_n, z1a, z1b, w_gate, w_up, w_down
    )
    far_rows = 2 * fk * slots
    far_part = call(far_body, (shape((far_rows, width), BF),) * 4, 8)(
        *chunks, waves[1], w_gate, w_up, w_down
    )

    def reduce(part):
        sent = exchange(part)
        total = part[0].astype(F32) + sent[1].astype(F32)
        return (total + sent[2].astype(F32) + sent[3].astype(F32)).astype(BF)

    sum_f = reduce(far_part)
    back = {}
    for i, k in enumerate(range(zs - 1, 1, -1)):
        back[k] = swap(sum_f[2 * slots * i : 2 * slots * (i + 1)], "ep", 2 * k)
    sum_n = reduce(near_part)
    next_own, next_other = [], []
    for at, k, got in ((2, 2, next_own), (3, 3, next_other)):
        got.append(swap(sum_n[at * slots : (at + 1) * slots], "ep", k))
    parts = [sum_n[: 2 * slots]] + [back[k] for k in range(2, zs)]
    mine = jnp.concatenate([p[:slots] for p in parts], axis=0)
    theirs = swap(jnp.concatenate([p[slots:] for p in parts], axis=0), "ep", 1)

    val = call(dense_out_body, shape((rows, width), F32), 8)(
        *hiddens, dense_out, side_gate
    )
    return call(combine_body, shape((rows, width), BF), 8)(
        mine, *next_own, theirs, *next_other, comb, val
    )


def general(
    tokens,
    gate_proj,
    up_proj,
    down_proj,
    side_input_weight,
    dense_out,
    dense_gate,
    chosen_rows,
    choice_weights,
):
    tok_rows = tokens.shape[0]
    width = tokens.shape[1] // lax.axis_size("tp")
    column_position = lax.axis_index("tp") * width
    own_cols = lax.dynamic_slice_in_dim(tokens, column_position, width, 1)
    expert_count, slot_rows = chosen_rows.shape
    capacity = expert_count * slot_rows
    picked = jnp.take(own_cols, chosen_rows.reshape(-1), axis=0).reshape(
        expert_count, slot_rows, width
    )
    arrived = lax.all_to_all(picked, "ep", split_axis=0, concat_axis=1, tiled=True).reshape(
        capacity, width
    )
    w_gate = gate_proj[0]
    w_up = up_proj[0]
    w_down = down_proj[0]
    piece = lax.all_gather(arrived, "tp", axis=1, tiled=True)
    gate_val = jnp.dot(piece, w_gate, preferred_element_type=jnp.float32)
    up_val = jnp.dot(piece, w_up, preferred_element_type=jnp.float32)
    hidden = (jax.nn.silu(gate_val) * up_val).astype(jnp.bfloat16)
    summed = lax.psum_scatter(
        lax.dot_general(
            w_down, hidden, (((0,), (1,)), ((), ())), preferred_element_type=jnp.float32
        ).astype(jnp.bfloat16),
        "tp",
        scatter_dimension=0,
        tiled=True,
    )
    returned = lax.all_to_all(summed, "ep", split_axis=1, concat_axis=1, tiled=True)
    hits = (
        chosen_rows.reshape(-1)[:, None] == jnp.arange(tok_rows, dtype=jnp.int32)[None, :]
    ).astype(jnp.bfloat16)
    scaled = returned.astype(jnp.float32) * choice_weights.reshape(-1)[None, :]
    high_part = scaled.astype(jnp.bfloat16)
    lower_half = (scaled - high_part.astype(jnp.float32)).astype(jnp.bfloat16)
    contract = (((0,), (1,)), ((), ()))
    routed = lax.dot_general(
        hits, high_part, contract, preferred_element_type=jnp.float32
    ) + lax.dot_general(hits, lower_half, contract, preferred_element_type=jnp.float32)
    dense_hidden = jax.nn.silu(
        jnp.dot(tokens, side_input_weight, preferred_element_type=jnp.float32)
    ).astype(jnp.bfloat16)
    dense_val = jnp.dot(
        lax.all_gather(dense_hidden, "tp", axis=1, tiled=True),
        dense_out,
        preferred_element_type=jnp.float32,
    )
    side_gate = jax.nn.sigmoid(jnp.dot(tokens, dense_gate, preferred_element_type=jnp.float32))
    return (routed + side_gate[:, None] * dense_val).astype(jnp.bfloat16)


def per_device(tokens, gate_proj, *rest):
    experts = lax.axis_size("ep")
    fits = (
        lax.axis_size("tp") == 4
        and experts >= 8
        and experts & (experts - 1) == 0
        and tokens.shape[1] % (4 * 128) == 0
        and gate_proj.shape[2] % 128 == 0
        and rest[2].shape[1] % 128 == 0
        and tokens.shape[0] <= 512
        and rest[5].size <= 512
    )
    if not fits:
        return general(tokens, gate_proj, *rest)
    return fast(tokens, gate_proj, *rest)


def solution(mesh):
    placed = (
        P("ep", None),
        P("ep", None, "tp"),
        P("ep", None, "tp"),
        P("ep", "tp", None),
        P(None, "tp"),
        P(None, "tp"),
        P(),
        P(None, "ep"),
        P(None, "ep"),
    )
    return jax.shard_map(
        per_device, mesh=mesh, in_specs=placed, out_specs=P("ep", "tp"), check_vma=False
    )
```
